32 devices in a mesh: tp: 8 (over z, y), dp: 4 (over x, core).
Axes of the slice: x: 2, y: 2, z: 4, core: 2. Of those that a mesh axis runs over, the one named last changes fastest.
Arguments:
- stream: bfloat16 [32, 4096], P('dp', 'tp'), may hold values from -6 to 6
- query_weight: bfloat16 [2, 4096, 3072], P(None, 'dp', 'tp'), may hold values from -0.09375 to 0.09375
- key_weight: bfloat16 [2, 4096, 3072], P(None, 'dp', 'tp'), may hold values from -0.09375 to 0.09375
- value_weight: bfloat16 [2, 4096, 3072], P(None, 'dp', 'tp'), may hold values from -0.09375 to 0.09375
- outgate_weight: bfloat16 [2, 4096, 3072], P(None, 'dp', 'tp'), may hold values from -0.09375 to 0.09375
- gate_weight: bfloat16 [2, 4096, 32], replicated, may hold values from -0.09375 to 0.09375
- gate_bias: float32 [2, 32], replicated, may hold values from -1 to 3
- output_weight: bfloat16 [2, 3072, 4096], P(None, 'dp', 'tp'), may hold values from -0.109375 to 0.109375
- norm_gain: float32 [2, 4096], replicated, may hold values from 0.1 to 1.9
- matrix_state: float32 [2, 32, 192, 16, 192], P(None, 'dp', 'tp'), may hold values from -0.6 to 0.6
- normalizer_state: float32 [2, 32, 16, 192], P(None, 'dp'), may hold values from -0.6 to 0.6
- stabilizer_state: float32 [2, 32, 16], P(None, 'dp'), may hold values from -4 to 4
Outputs:
- out_stream: bfloat16 [32, 4096], P('dp', 'tp')
- new_matrix: float32 [2, 32, 192, 16, 192], P(None, 'dp', 'tp')
- new_normalizer: float32 [2, 32, 16, 192], P(None, 'dp')
- new_stabilizer: float32 [2, 32, 16], P(None, 'dp')
The draws below stay inside these ranges and needn't reach their ends.
All inputs are finite; a program needn't handle non-finite values.
Results may differ from the reference program's by a relative error of at most 0.015.
Values may be sent and summed in bfloat16 or wider, within the bound.
A program may use at most 128 MiB of HBM per device.

```python
import jax
import jax.numpy as jnp
from jax import lax

D = 4096
HEADS = 16
HEAD_DIM = 192
BLOCKS = 2
SEQS = 32
VALUE_WIDTH = 3072


def steps_of(key, shape, shards, smallest, high):
    def one(axis_at, blocks):
        steps = jax.random.uniform(jax.random.fold_in(jax.random.fold_in(key, 6), axis_at), (blocks,), jnp.float32, smallest / len(shards), high / len(shards))
        return jnp.repeat(jnp.exp(steps), shape[axis_at] // blocks).reshape((-1,) + (1,) * (len(shape) - axis_at - 1))

    level = one(*shards[0])
    for cut in shards[1:]:
        level = level * one(*cut)
    return level


def scatter_about(key, dims, scale, reach, cuts=(), held_as=jnp.bfloat16):
    entries = jax.random.normal(key, dims, jnp.float32) * scale
    if len(cuts) > 0:
        entries = steps_of(key, dims, cuts, -0.22, 0.18) * entries
    return jnp.clip(entries, min=-reach, max=reach).astype(held_as)


def setup_inputs(seed: int = 0) -> dict:
    key_list = jax.random.split(jax.random.key(seed), 13)
    stream = scatter_about(key_list[0], (SEQS, D), 1.0, 6.0, ((0, 4), (1, 8)))
    query_weight = scatter_about(key_list[1], (BLOCKS, D, VALUE_WIDTH), D ** -0.5, 0.09375, ((1, 4), (2, 8)))
    key_weight = scatter_about(key_list[2], (BLOCKS, D, VALUE_WIDTH), D ** -0.5, 0.09375, ((1, 4), (2, 8)))
    value_weight = scatter_about(key_list[3], (BLOCKS, D, VALUE_WIDTH), D ** -0.5, 0.09375, ((1, 4), (2, 8)))
    outgate_weight = scatter_about(key_list[4], (BLOCKS, D, VALUE_WIDTH), D ** -0.5, 0.09375, ((1, 4), (2, 8)))
    gate_weight = scatter_about(key_list[5], (BLOCKS, D, 2 * HEADS), D ** -0.5, 0.09375)
    gate_bias = jnp.clip(jax.random.uniform(key_list[6], (BLOCKS, 2 * HEADS), jnp.float32, -1.0, 3.0), -1.0, 3.0)
    output_weight = scatter_about(key_list[7], (BLOCKS, VALUE_WIDTH, D), VALUE_WIDTH ** -0.5, 0.109375, ((1, 4), (2, 8)))
    norm_gain = jnp.clip(1.0 + 0.18 * jax.random.normal(key_list[8], (BLOCKS, D), jnp.float32), 0.1, 1.9)
    matrix_state = scatter_about(key_list[9], (BLOCKS, SEQS, HEAD_DIM, HEADS, HEAD_DIM), 0.1, 0.6, ((1, 4), (2, 8)), jnp.float32)
    normalizer_state = scatter_about(key_list[10], (BLOCKS, SEQS, HEADS, HEAD_DIM), 0.1, 0.6, ((1, 4),), jnp.float32)
    stabilizer_state = scatter_about(key_list[11], (BLOCKS, SEQS, HEADS), 1.0, 4.0, ((1, 4),), jnp.float32)
    return {"stream": stream, "query_weight": query_weight, "key_weight": key_weight, "value_weight": value_weight, "outgate_weight": outgate_weight, "gate_weight": gate_weight, "gate_bias": gate_bias, "output_weight": output_weight, "norm_gain": norm_gain, "matrix_state": matrix_state, "normalizer_state": normalizer_state, "stabilizer_state": stabilizer_state}


residual_scale = 8.0 ** 0.25
norm_eps = 1e-05

def normalize(values_in, gain):
    upcast = values_in.astype(jnp.float32)
    average = lax.optimization_barrier(jnp.mean(upcast, axis=-1, keepdims=True))
    variance = lax.optimization_barrier(jnp.mean(jnp.square(upcast - average), axis=-1, keepdims=True))
    return ((upcast - average) * lax.rsqrt(variance + norm_eps) * gain).astype(jnp.bfloat16)

def reference(stream, query_weight, key_weight, value_weight, outgate_weight, gate_weight, gate_bias, output_weight, norm_gain, matrix_state, normalizer_state, stabilizer_state):
    seq_count = stream.shape[0]
    current = stream
    new_mats, new_norms, new_stabs = ([], [], [])
    for block_no in range(BLOCKS):
        query = jnp.dot(current, query_weight[block_no], preferred_element_type=jnp.float32).astype(jnp.bfloat16)
        key_vec = jnp.dot(current, key_weight[block_no], preferred_element_type=jnp.float32).astype(jnp.bfloat16)
        value = jnp.dot(current, value_weight[block_no], preferred_element_type=jnp.float32).astype(jnp.bfloat16)
        outgate = jnp.dot(current, outgate_weight[block_no], preferred_element_type=jnp.float32).astype(jnp.bfloat16)
        gate_pre = jnp.dot(current, gate_weight[block_no], preferred_element_type=jnp.float32) + gate_bias[block_no]
        log_in = gate_pre[:, :HEADS]
        log_forget = jax.nn.log_sigmoid(gate_pre[:, HEADS:])
        old_stab = stabilizer_state[block_no]
        stab_new = jnp.maximum(log_forget + old_stab, log_in)
        retain = jnp.exp(log_forget + old_stab - stab_new)
        admit = jnp.exp(log_in - stab_new)
        queries = query.astype(jnp.float32).reshape(seq_count, HEADS, HEAD_DIM)
        keys = key_vec.astype(jnp.float32).reshape(seq_count, HEADS, HEAD_DIM) * HEAD_DIM ** (-0.5)
        values = value.astype(jnp.float32).reshape(seq_count, HEAD_DIM, HEADS)
        matrix = retain[:, None, :, None] * matrix_state[block_no] + admit[:, None, :, None] * values[..., None] * keys[:, None, :, :]
        norm_new = retain[..., None] * normalizer_state[block_no] + admit[..., None] * keys
        numerator = jnp.einsum('shd,sehd->seh', queries, matrix, precision=lax.Precision.HIGHEST)
        denominator = lax.optimization_barrier(jnp.sum(queries * norm_new, axis=-1))
        divisor = jnp.maximum(jnp.abs(denominator), 1.0)
        readout = (numerator / divisor[:, None, :]).reshape(seq_count, HEADS * HEAD_DIM)
        hidden = (readout * jax.nn.sigmoid(outgate.astype(jnp.float32))).astype(jnp.bfloat16)
        branch = jnp.dot(hidden, output_weight[block_no], preferred_element_type=jnp.float32)
        summed = (residual_scale * current.astype(jnp.float32) + branch).astype(jnp.bfloat16)
        current = normalize(summed, norm_gain[block_no])
        new_mats.append(matrix)
        new_norms.append(norm_new)
        new_stabs.append(stab_new)
    return (current, jnp.stack(new_mats), jnp.stack(new_norms), jnp.stack(new_stabs))
```

```python
import functools
import math

import jax
import jax.numpy as jnp
from jax import lax
from jax.experimental import pallas as pl
from jax.experimental.pallas import tpu as pltpu
from jax.sharding import PartitionSpec as P

residual_scale = 8.0**0.25
norm_eps = 1e-05
f32, bf16 = jnp.float32, jnp.bfloat16
STREAM, QK, GATE, VO, HEAD, HID, OUT, STAT = range(8)


def each(count, step):
    if count <= 8:
        for k in range(count):
            step(k)
    else:

        def body(k, carry):
            step(k)
            return carry

        lax.fori_loop(0, count, body, 0)


def kernel(
    tp,
    dp,
    stream,
    wq,
    wk,
    wv,
    wo,
    gate_weight,
    gate_bias,
    out_weight,
    norm_gain,
    matrix_in,
    normal_in,
    stab_in,
    stream_out,
    matrix_out,
    normal_out,
    stab_out,
    x_own,
    w_in,
    w_gate,
    bias,
    w_out,
    gain,
    matrix,
    normal,
    stab,
    x_all,
    qk_part,
    qk_recv,
    g_part,
    g_recv,
    vo_part,
    vo_recv,
    head_own,
    head_all,
    hid_own,
    hid_all,
    out_part,
    out_recv,
    stat_own,
    stat_all,
    y_own,
    queries_ref,
    keys_ref,
    result,
    load_sem,
    store_sem,
    send_sem,
    recv_sem,
):
    blocks, seqs, chans, heads, size = matrix.shape
    feats = x_own.shape[1]
    cols = w_in.shape[3]
    ratio = tp // dp
    width = head_all.shape[-1]
    pieces = cols // width
    per_head = size // width
    ti, di = lax.axis_index("tp"), lax.axis_index("dp")
    group = ti // ratio
    place = ti - group * ratio
    home = group == di
    model = tp * feats

    loads = []

    def load(src, dst):
        copy = pltpu.make_async_copy(src, dst, load_sem.at[len(loads)])
        copy.start()
        loads.append(copy)
        return copy

    rows = w_gate.shape[1]
    got_x = load(stream, x_own)
    got_w, got_gate, got_out, got_matrix = [], [], [], []
    for b in range(blocks):
        got_w.append([load(w.at[b], w_in.at[b, n]) for n, w in enumerate((wq, wk, wv, wo))])
        got_gate.append(load(gate_weight.at[b, pl.ds(pl.multiple_of(di * rows, rows), rows)], w_gate.at[b]))
        if b == 0:
            got_small = [load(gate_bias, bias), load(norm_gain, gain), load(normal_in, normal), load(stab_in, stab)]
        got_matrix.append(load(matrix_in.at[b], matrix.at[b]))
        got_out.append(load(out_weight.at[b], w_out.at[b]))

    barrier = pltpu.get_barrier_semaphore()

    def greet(k):
        other = lax.rem(ti * dp + di + 1 + k, tp * dp)
        pl.semaphore_signal(
            barrier,
            inc=1,
            device_id={"tp": other // dp, "dp": lax.rem(other, dp)},
            device_id_type=pl.DeviceIdType.MESH,
        )

    each(tp * dp - 1, greet)
    pl.semaphore_wait(barrier, tp * dp - 1)

    unsent = []

    def send(src, dst, b, phase, where):
        pltpu.make_async_remote_copy(
            src_ref=src,
            dst_ref=dst,
            send_sem=send_sem.at[b, phase],
            recv_sem=recv_sem.at[b, phase],
            device_id=where,
            device_id_type=pl.DeviceIdType.MESH,
        ).start()

    def await_bytes(ref, sem):
        pltpu.make_async_copy(ref, ref, sem).wait()

    def to_tp(src, dst, b, phase):
        each(tp - 1, lambda k: send(src, dst, b, phase, {"tp": lax.rem(ti + 1 + k, tp), "dp": di}))
        unsent.append((tp - 1, src, b, phase, None))

    def to_dp(part, recv, b, phase):
        def one(k):
            other = lax.rem(di + 1 + k, dp)
            send(part.at[b, other], recv.at[b, di], b, phase, {"tp": ti, "dp": other})

        each(dp - 1, one)
        unsent.append((dp - 1, part.at[b, 0], b, phase, None))

    def to_group(src, slots, b, phase):
        dst = slots.at[b, place * dp + di]

        def one(k):
            send(src, dst, b, phase, {"tp": lax.rem(ti + 1 + k, tp), "dp": group})

        each(tp - 1, one)

        @pl.when(jnp.logical_not(home))
        def _():
            send(src, dst, b, phase, {"tp": ti, "dp": group})

        @pl.when(home)
        def _():
            slots[b, place * dp + di] = src[...]

        unsent.append((tp - 1, src, b, phase, jnp.logical_not(home)))

    def from_group(slots, b, phase):
        @pl.when(home)
        def _():
            await_bytes(slots.at[b, pl.ds(0, tp - 1)], recv_sem.at[b, phase])

        @pl.when(jnp.logical_not(home))
        def _():
            await_bytes(slots.at[b], recv_sem.at[b, phase])

    def rows_of(slots, b, c):
        held = slots[b, c * dp : (c + 1) * dp].astype(f32)
        return held.reshape(dp * seqs, held.shape[-1])

    def moments(stats):
        means, squares = stats[..., 0:1], stats[..., 1:2]
        mean = jnp.sum(means, axis=-3) * (1.0 / tp)
        apart = means - jnp.expand_dims(mean, -3)
        variance = (jnp.sum(squares, axis=-3) + feats * jnp.sum(apart * apart, axis=-3)) * (1.0 / model)
        return mean, lax.rsqrt(variance + norm_eps)

    def gain_of(b, chunk):
        if len(gain.shape) == 2:
            return gain[b : b + 1, pl.ds(pl.multiple_of(chunk * feats, feats), feats)]
        return gain[b, pl.ds(chunk, 1), :]

    got_x.wait()
    to_group(x_own, x_all, 0, STREAM)
    own = x_own[...].astype(f32)
    outs = []

    def store(src, dst):
        copy = pltpu.make_async_copy(src, dst, store_sem.at[len(outs)])
        copy.start()
        outs.append(copy)

    for b in range(blocks):
        if b == 0:
            for copy in got_w[b][:2]:
                copy.wait()
        from_group(x_all, b, STREAM)
        chunks = [rows_of(x_all, b, c) for c in range(ratio)]
        if b > 0:
            await_bytes(stat_all.at[b - 1, pl.ds(0, tp * dp - 1)], recv_sem.at[b - 1, STAT])
            mean, scale = moments(stat_all[b - 1].reshape(dp, tp, seqs, 128))
            mean, scale = mean.reshape(dp * seqs, 1), scale.reshape(dp * seqs, 1)
            chunks = [
                (chunk - mean) * scale * gain_of(b - 1, di * ratio + c) for c, chunk in enumerate(chunks)
            ]
        chunks = [chunk.astype(bf16) for chunk in chunks]

        def project(w, depth=feats):
            return sum(
                jnp.dot(chunk, w[c * depth : (c + 1) * depth, :], preferred_element_type=f32)
                for c, chunk in enumerate(chunks)
            )

        if b > 0:
            for copy in got_w[b][:2]:
                copy.wait()
        for n in range(2):
            qk_part[b, :, n] = project(w_in.at[b, n]).reshape(dp, seqs, cols)
        qk_recv[b, di] = qk_part[b, di]
        to_dp(qk_part, qk_recv, b, QK)
        got_gate[b].wait()
        g_part[b] = project(w_gate.at[b]).reshape(dp, seqs, 2 * heads)
        g_recv[b, di] = g_part[b, di]
        to_dp(g_part, g_recv, b, GATE)
        for copy in got_w[b][2:]:
            copy.wait()
        for n in range(2):
            vo_part[b, :, n] = project(w_in.at[b, 2 + n]).reshape(dp, seqs, cols)
        vo_recv[b, di] = vo_part[b, di]
        to_dp(vo_part, vo_recv, b, VO)
        if b > 0:
            m_own, s_own = moments(stat_all[b - 1, pl.ds(di * tp, tp)])
            own = ((y_own[b - 1].astype(f32) - m_own) * s_own * gain_of(b - 1, ti)).astype(bf16).astype(f32)

        await_bytes(qk_recv.at[b, pl.ds(0, dp - 1)], recv_sem.at[b, QK])
        for n in range(2):
            total = jnp.sum(qk_recv[b, :, n], axis=0)
            for p in range(pieces):
                head_own[b, n, p] = total[:, p * width : (p + 1) * width].astype(bf16)
        head_all[b, ti] = head_own[b]
        to_tp(head_own.at[b], head_all.at[b, ti], b, HEAD)

        await_bytes(g_recv.at[b, pl.ds(0, dp - 1)], recv_sem.at[b, GATE])
        if b == 0:
            for copy in got_small:
                copy.wait()
        pre = jnp.sum(g_recv[b], axis=0) + bias[b : b + 1, :]
        log_in = pre[:, :heads]
        raw = pre[:, heads:]
        log_forget = jnp.minimum(raw, 0.0) - jnp.log1p(jnp.exp(-jnp.abs(raw)))
        carried = log_forget + stab[b]
        stab_new = jnp.maximum(carried, log_in)
        stab[b] = stab_new
        retain = jnp.exp(carried - stab_new).T
        admit = jnp.exp(log_in - stab_new).T
        await_bytes(vo_recv.at[b, pl.ds(0, dp - 1)], recv_sem.at[b, VO])
        value = jnp.sum(vo_recv[b, :, 0], axis=0).astype(bf16).astype(f32).T
        outgate = jnp.sum(vo_recv[b, :, 1], axis=0).astype(bf16).astype(f32)
        opened = jax.nn.sigmoid(outgate)
        got_matrix[b].wait()

        await_bytes(head_all.at[b, pl.ds(0, tp - 1)], recv_sem.at[b, HEAD])
        for h in range(heads):
            for n, ref in ((0, queries_ref), (1, keys_ref)):
                parts = [
                    head_all[b, g // pieces, n, g % pieces].astype(f32)
                    for g in range(h * per_head, (h + 1) * per_head)
                ]
                whole = parts[0] if per_head == 1 else jnp.concatenate(parts, axis=-1)
                if n == 1:
                    whole = whole * size ** (-0.5)
                ref[:, h, :] = whole

        lane = lax.broadcasted_iota(jnp.int32, (chans * heads, seqs), 1)
        readout = jnp.zeros((chans * heads, seqs), f32)
        for s in range(seqs):
            q, k = queries_ref[s], keys_ref[s]
            keep, take = retain[:, s : s + 1], admit[:, s : s + 1]
            norm_new = keep * normal[b, s] + take * k
            normal[b, s] = norm_new
            divisor = jnp.maximum(jnp.abs(jnp.sum(q * norm_new, axis=-1, keepdims=True)), 1.0)
            v = value[:, s : s + 1].reshape(chans, heads, 1)
            new = keep[None] * matrix[b, s] + (take[None] * v) * k[None]
            matrix[b, s] = new
            read = jnp.sum(q[None] * new, axis=-1, keepdims=True) / divisor[None]
            readout = jnp.where(lane == s, read.reshape(chans * heads, 1), readout)
        hid_own[b] = (readout.T * opened).astype(bf16)
        to_group(hid_own.at[b], hid_all, b, HID)
        store(matrix.at[b], matrix_out.at[b])

        got_out[b].wait()
        from_group(hid_all, b, HID)
        chunks = [rows_of(hid_all, b, c).astype(bf16) for c in range(ratio)]
        out_part[b] = project(w_out.at[b], cols).reshape(dp, seqs, feats)
        out_recv[b, di] = out_part[b, di]
        to_dp(out_part, out_recv, b, OUT)
        await_bytes(out_recv.at[b, pl.ds(0, dp - 1)], recv_sem.at[b, OUT])
        y = (residual_scale * own + jnp.sum(out_recv[b], axis=0)).astype(bf16)
        y_own[b] = y
        if b + 1 < blocks:
            to_group(y_own.at[b], x_all, b + 1, STREAM)
        y = y.astype(f32)
        mean = jnp.mean(y, axis=-1, keepdims=True)
        square = jnp.sum(jnp.square(y - mean), axis=-1, keepdims=True)
        at = lax.broadcasted_iota(jnp.int32, (seqs, 128), 1)
        stat = jnp.where(at == 0, mean, square)
        stat_own[b] = stat
        stat_all[b, di * tp + ti] = stat

        if b + 1 < blocks:

            def tell(k, b=b):
                other = lax.rem(ti * dp + di + 1 + k, tp * dp)
                send(
                    stat_own.at[b],
                    stat_all.at[b, di * tp + ti],
                    b,
                    STAT,
                    {"tp": other // dp, "dp": lax.rem(other, dp)},
                )

            each(tp * dp - 1, tell)
            unsent.append((tp * dp - 1, stat_own.at[b], b, STAT, None))
        else:
            to_tp(stat_own.at[b], stat_all.at[b, di * tp + ti], b, STAT)
            store(normal, normal_out)
            store(stab, stab_out)
            await_bytes(stat_all.at[b, pl.ds(0, tp - 1)], recv_sem.at[b, STAT])
            mean, scale = moments(stat_all[b, pl.ds(di * tp, tp)])
            result[...] = ((y - mean) * scale * gain_of(b, ti)).astype(bf16)
            store(result, stream_out)

    for count, src, b, phase, also in unsent:
        each(count, lambda k: await_bytes(src, send_sem.at[b, phase]))
        if also is not None:

            @pl.when(also)
            def _():
                await_bytes(src, send_sem.at[b, phase])

    for copy in outs:
        copy.wait()


def shards(
    tp,
    dp,
    stream,
    query_weight,
    key_weight,
    value_weight,
    outgate_weight,
    gate_weight,
    gate_bias,
    output_weight,
    norm_gain,
    matrix_state,
    normalizer_state,
    stabilizer_state,
):
    blocks, seqs, chans, heads, size = matrix_state.shape
    feats = stream.shape[1]
    _, rows, cols = query_weight.shape
    ratio = tp // dp
    width = math.gcd(cols, size)
    pieces = cols // width
    if feats % 128:
        norm_gain = norm_gain.reshape(blocks, tp, feats)
    vmem = pltpu.VMEM
    anywhere = pl.BlockSpec(memory_space=pl.ANY)
    scratch = [
        vmem((seqs, feats), bf16),
        vmem((blocks, 4, rows, cols), bf16),
        vmem((blocks, rows, 2 * heads), bf16),
        vmem(gate_bias.shape, f32),
        vmem(output_weight.shape, bf16),
        vmem(norm_gain.shape, f32),
        vmem(matrix_state.shape, f32),
        vmem(normalizer_state.shape, f32),
        vmem(stabilizer_state.shape, f32),
        vmem((blocks, ratio * dp, seqs, feats), bf16),
        vmem((blocks, dp, 2, seqs, cols), f32),
        vmem((blocks, dp, 2, seqs, cols), f32),
        vmem((blocks, dp, seqs, 2 * heads), f32),
        vmem((blocks, dp, seqs, 2 * heads), f32),
        vmem((blocks, dp, 2, seqs, cols), f32),
        vmem((blocks, dp, 2, seqs, cols), f32),
        vmem((blocks, 2, pieces, seqs, width), bf16),
        vmem((blocks, tp, 2, pieces, seqs, width), bf16),
        vmem((blocks, seqs, cols), bf16),
        vmem((blocks, ratio * dp, seqs, cols), bf16),
        vmem((blocks, dp, seqs, feats), f32),
        vmem((blocks, dp, seqs, feats), f32),
        vmem((blocks, seqs, 128), f32),
        vmem((blocks, dp * tp, seqs, 128), f32),
        vmem((blocks, seqs, feats), bf16),
        vmem((seqs, heads, size), f32),
        vmem((seqs, heads, size), f32),
        vmem((seqs, feats), bf16),
        pltpu.SemaphoreType.DMA((5 + 7 * blocks,)),
        pltpu.SemaphoreType.DMA((3 + blocks,)),
        pltpu.SemaphoreType.DMA((blocks, 8)),
        pltpu.SemaphoreType.DMA((blocks, 8)),
    ]
    return pl.pallas_call(
        functools.partial(kernel, tp, dp),
        out_shape=(
            jax.ShapeDtypeStruct(stream.shape, stream.dtype),
            jax.ShapeDtypeStruct(matrix_state.shape, f32),
            jax.ShapeDtypeStruct(normalizer_state.shape, f32),
            jax.ShapeDtypeStruct(stabilizer_state.shape, f32),
        ),
        in_specs=[anywhere] * 12,
        out_specs=(anywhere,) * 4,
        scratch_shapes=scratch,
        compiler_params=pltpu.CompilerParams(
            collective_id=0, has_side_effects=True, vmem_limit_bytes=60 * 1024 * 1024
        ),
    )(
        stream,
        query_weight,
        key_weight,
        value_weight,
        outgate_weight,
        gate_weight,
        gate_bias,
        output_weight,
        norm_gain,
        matrix_state,
        normalizer_state,
        stabilizer_state,
    )


def solution(mesh):
    return jax.shard_map(
        functools.partial(shards, mesh.shape["tp"], mesh.shape["dp"]),
        mesh=mesh,
        in_specs=(
            P("dp", "tp"),
            P(None, "dp", "tp"),
            P(None, "dp", "tp"),
            P(None, "dp", "tp"),
            P(None, "dp", "tp"),
            P(),
            P(),
            P(None, "dp", "tp"),
            P(),
            P(None, "dp", "tp", None, None),
            P(None, "dp", None, None),
            P(None, "dp", None),
        ),
        out_specs=(
            P("dp", "tp"),
            P(None, "dp", "tp", None, None),
            P(None, "dp", None, None),
            P(None, "dp", None),
        ),
        check_vma=False,
    )
```

```python
import functools
import math

import jax
import jax.numpy as jnp
from jax import lax
from jax.experimental import pallas as pl
from jax.experimental.pallas import tpu as pltpu
from jax.sharding import PartitionSpec as P

residual_scale = 8.0**0.25
norm_eps = 1e-05
f32, bf16 = jnp.float32, jnp.bfloat16
STREAM, QK, GATE, VO, HEAD, HID, OUT, STAT = range(8)


def each(count, step):
    if count <= 8:
        for k in range(count):
            step(k)
    else:

        def body(k, carry):
            step(k)
            return carry

        lax.fori_loop(0, count, body, 0)


def kernel(
    tp,
    dp,
    stream,
    wq,
    wk,
    wv,
    wo,
    gate_weight,
    gate_bias,
    out_weight,
    norm_gain,
    matrix_in,
    normal_in,
    stab_in,
    result,
    matrix,
    normal,
    stab,
    x_own,
    w_in,
    w_gate,
    bias,
    w_out,
    gain,
    x_all,
    qk_part,
    qk_recv,
    g_part,
    g_recv,
    vo_part,
    vo_recv,
    head_own,
    head_all,
    hid_own,
    hid_all,
    out_part,
    out_recv,
    stat_own,
    stat_all,
    y_own,
    queries_ref,
    keys_ref,
    load_sem,
    send_sem,
    recv_sem,
):
    blocks, seqs, chans, heads, size = matrix.shape
    feats = x_own.shape[1]
    cols = w_in.shape[3]
    ratio = tp // dp
    width = head_all.shape[-1]
    pieces = cols // width
    per_head = size // width
    ti, di = lax.axis_index("tp"), lax.axis_index("dp")
    group = ti // ratio
    place = ti - group * ratio
    home = group == di
    model = tp * feats

    loads = []

    def load(src, dst):
        copy = pltpu.make_async_copy(src, dst, load_sem.at[len(loads)])
        copy.start()
        loads.append(copy)
        return copy

    rows = w_gate.shape[2]
    got_x = load(stream, x_own)
    got_w, got_gate, got_out, got_matrix = [], [], [], []
    for b in range(blocks):
        got_w.append([load(w.at[b], w_in.at[b, n]) for n, w in enumerate((wq, wk, wv, wo))])
        got_gate.append(load(gate_weight.at[b, :, pl.ds(pl.multiple_of(di * rows, rows), rows)], w_gate.at[b]))
        if b == 0:
            got_small = [load(gate_bias, bias), load(norm_gain, gain), load(normal_in, normal), load(stab_in, stab)]
        got_matrix.append(load(matrix_in.at[b], matrix.at[b]))
        got_out.append(load(out_weight.at[b], w_out.at[b]))

    barrier = pltpu.get_barrier_semaphore()

    def greet(where):
        pl.semaphore_signal(barrier, inc=1, device_id=where, device_id_type=pl.DeviceIdType.MESH)

    def to_others(tell):
        def along(t, first):
            each(dp - first, lambda d: tell({"tp": t, "dp": lax.rem(di + first + d, dp)}))

        each(tp - 1, lambda k: along(lax.rem(ti + 1 + k, tp), 0))
        along(ti, 1)

    to_others(greet)
    pl.semaphore_wait(barrier, tp * dp - 1)

    unsent = []

    def send(src, dst, b, phase, where):
        pltpu.make_async_remote_copy(
            src_ref=src,
            dst_ref=dst,
            send_sem=send_sem.at[b, phase],
            recv_sem=recv_sem.at[b, phase],
            device_id=where,
            device_id_type=pl.DeviceIdType.MESH,
        ).start()

    def await_bytes(ref, sem):
        pltpu.make_async_copy(ref, ref, sem).wait()

    def to_tp(src, dst, b, phase):
        each(tp - 1, lambda k: send(src, dst, b, phase, {"tp": lax.rem(ti + 1 + k, tp), "dp": di}))
        unsent.append((tp - 1, src, b, phase, None))

    def to_dp(part, recv, b, phase):
        def one(k):
            other = lax.rem(di + 1 + k, dp)
            send(part.at[b, other], recv.at[b, di], b, phase, {"tp": ti, "dp": other})

        each(dp - 1, one)
        unsent.append((dp - 1, part.at[b, 0], b, phase, None))

    def to_group(src, slots, b, phase):
        dst = slots.at[b, place * dp + di]

        def one(k):
            send(src, dst, b, phase, {"tp": lax.rem(ti + 1 + k, tp), "dp": group})

        each(tp - 1, one)

        @pl.when(jnp.logical_not(home))
        def _():
            send(src, dst, b, phase, {"tp": ti, "dp": group})

        @pl.when(home)
        def _():
            slots[b, place * dp + di] = src[...]

        unsent.append((tp - 1, src, b, phase, jnp.logical_not(home)))

    def from_group(slots, b, phase):
        @pl.when(home)
        def _():
            await_bytes(slots.at[b, pl.ds(0, tp - 1)], recv_sem.at[b, phase])

        @pl.when(jnp.logical_not(home))
        def _():
            await_bytes(slots.at[b], recv_sem.at[b, phase])

    def rows_of(slots, b, c):
        held = slots[b, c * dp : (c + 1) * dp].astype(f32)
        return held.reshape(dp * seqs, held.shape[-1])

    def moments(stats):
        def column(row, at):
            shape = (seqs, row.shape[-1])
            pick = lax.broadcasted_iota(jnp.int32, shape, 1) == lax.broadcasted_iota(jnp.int32, shape, 0) + at
            return jnp.sum(jnp.where(pick, jnp.broadcast_to(row, shape), 0.0), axis=-1, keepdims=True)

        sums = jnp.sum(stats, axis=0)
        apart = stats - sums[None] * (1.0 / tp)
        spread = jnp.sum(apart * apart, axis=0)
        variance = (column(sums, seqs) + feats * column(spread, 0)) * (1.0 / model)
        return column(sums, 0) * (1.0 / tp), lax.rsqrt(variance + norm_eps)

    def gain_of(b, chunk):
        if len(gain.shape) == 2:
            return gain[b : b + 1, pl.ds(pl.multiple_of(chunk * feats, feats), feats)]
        return gain[b, pl.ds(chunk, 1), :]

    got_x.wait()
    to_group(x_own, x_all, 0, STREAM)
    own = x_own[...].astype(f32)

    for b in range(blocks):
        if b == 0:
            for copy in got_w[b][:2]:
                copy.wait()
        from_group(x_all, b, STREAM)
        chunks = [rows_of(x_all, b, c) for c in range(ratio)]
        if b > 0:
            await_bytes(stat_all.at[b - 1, pl.ds(0, tp * dp - 1)], recv_sem.at[b - 1, STAT])
            pairs = [moments(stat_all[b - 1, i * tp : (i + 1) * tp]) for i in range(dp)]
            mean, scale = (jnp.concatenate(columns, axis=0) for columns in zip(*pairs))
            chunks = [
                (chunk - mean) * scale * gain_of(b - 1, di * ratio + c) for c, chunk in enumerate(chunks)
            ]
        chunks = [chunk.astype(bf16) for chunk in chunks]

        def project(w, depth=feats):
            return sum(
                jnp.dot(chunk, w[c * depth : (c + 1) * depth, :], preferred_element_type=f32)
                for c, chunk in enumerate(chunks)
            )

        if b > 0:
            for copy in got_w[b][:2]:
                copy.wait()
        for n in range(2):
            qk_part[b, :, n] = project(w_in.at[b, n]).reshape(dp, seqs, cols).astype(bf16)
        qk_recv[b, di] = qk_part[b, di]
        to_dp(qk_part, qk_recv, b, QK)
        got_gate[b].wait()
        pre = lax.dot_general(
            jnp.concatenate(chunks, axis=-1), w_gate[b], (((1,), (1,)), ((), ())), preferred_element_type=f32
        )
        g_part[b] = pre.reshape(dp, seqs, 2 * heads)
        g_recv[b, di] = g_part[b, di]
        to_dp(g_part, g_recv, b, GATE)
        for copy in got_w[b][2:]:
            copy.wait()
        for n in range(2):
            vo_part[b, :, n] = project(w_in.at[b, 2 + n]).reshape(dp, seqs, cols).astype(bf16)
        vo_recv[b, di] = vo_part[b, di]
        to_dp(vo_part, vo_recv, b, VO)
        if b > 0:
            m_own, s_own = moments(stat_all[b - 1, pl.ds(di * tp, tp)])
            own = ((y_own[b - 1].astype(f32) - m_own) * s_own * gain_of(b - 1, ti)).astype(bf16).astype(f32)

        await_bytes(qk_recv.at[b, pl.ds(0, dp - 1)], recv_sem.at[b, QK])
        for n in range(2):
            total = jnp.sum(qk_recv[b, :, n].astype(f32), axis=0)
            for p in range(pieces):
                head_own[b, n, p] = total[:, p * width : (p + 1) * width].astype(bf16)
        head_all[b, ti] = head_own[b]
        to_tp(head_own.at[b], head_all.at[b, ti], b, HEAD)

        await_bytes(g_recv.at[b, pl.ds(0, dp - 1)], recv_sem.at[b, GATE])
        if b == 0:
            for copy in got_small:
                copy.wait()
        pre = jnp.sum(g_recv[b], axis=0) + bias[b : b + 1, :]
        log_in = pre[:, :heads]
        raw = pre[:, heads:]
        log_forget = jnp.minimum(raw, 0.0) - jnp.log1p(jnp.exp(-jnp.abs(raw)))
        carried = log_forget + stab[b]
        stab_new = jnp.maximum(carried, log_in)
        stab[b] = stab_new
        retain = jnp.exp(carried - stab_new).T
        admit = jnp.exp(log_in - stab_new).T
        await_bytes(vo_recv.at[b, pl.ds(0, dp - 1)], recv_sem.at[b, VO])
        value = jnp.sum(vo_recv[b, :, 0].astype(f32), axis=0).astype(bf16).astype(f32).T
        outgate = jnp.sum(vo_recv[b, :, 1].astype(f32), axis=0).astype(bf16).astype(f32)
        opened = jax.nn.sigmoid(outgate)
        got_matrix[b].wait()

        await_bytes(head_all.at[b, pl.ds(0, tp - 1)], recv_sem.at[b, HEAD])
        for h in range(heads):
            for n, ref in ((0, queries_ref), (1, keys_ref)):
                parts = [
                    head_all[b, g // pieces, n, g % pieces].astype(f32)
                    for g in range(h * per_head, (h + 1) * per_head)
                ]
                whole = parts[0] if per_head == 1 else jnp.concatenate(parts, axis=-1)
                if n == 1:
                    whole = whole * size ** (-0.5)
                ref[:, h, :] = whole

        lane = lax.broadcasted_iota(jnp.int32, (chans * heads, seqs), 1)
        readout = jnp.zeros((chans * heads, seqs), f32)
        for s in range(seqs):
            q, k = queries_ref[s], keys_ref[s]
            keep, take = retain[:, s : s + 1], admit[:, s : s + 1]
            norm_new = keep * normal[b, s] + take * k
            normal[b, s] = norm_new
            divisor = jnp.maximum(jnp.abs(jnp.sum(q * norm_new, axis=-1, keepdims=True)), 1.0)
            v = value[:, s : s + 1].reshape(chans, heads, 1)
            new = keep[None] * matrix[b, s] + (take[None] * v) * k[None]
            matrix[b, s] = new
            read = jnp.sum(q[None] * new, axis=-1, keepdims=True) / divisor[None]
            readout = jnp.where(lane == s, read.reshape(chans * heads, 1), readout)
        hid_own[b] = (readout.T * opened).astype(bf16)
        to_group(hid_own.at[b], hid_all, b, HID)

        got_out[b].wait()
        from_group(hid_all, b, HID)
        chunks = [rows_of(hid_all, b, c).astype(bf16) for c in range(ratio)]
        out_part[b] = project(w_out.at[b], cols).reshape(dp, seqs, feats).astype(bf16)
        out_recv[b, di] = out_part[b, di]
        to_dp(out_part, out_recv, b, OUT)
        await_bytes(out_recv.at[b, pl.ds(0, dp - 1)], recv_sem.at[b, OUT])
        y = (residual_scale * own + jnp.sum(out_recv[b].astype(f32), axis=0)).astype(bf16)
        y_own[b] = y
        if b + 1 < blocks:
            to_group(y_own.at[b], x_all, b + 1, STREAM)
        y = y.astype(f32)
        mean = jnp.mean(y, axis=-1, keepdims=True)
        square = jnp.sum(jnp.square(y - mean), axis=-1, keepdims=True)
        lanes = lax.broadcasted_iota(jnp.int32, (seqs, 128), 1)
        seq = lax.broadcasted_iota(jnp.int32, (seqs, 128), 0)
        stat = jnp.where(lanes == seq, mean, jnp.where(lanes == seq + seqs, square, 0.0))
        stat = jnp.sum(stat, axis=0, keepdims=True)
        stat_own[b] = stat
        stat_all[b, di * tp + ti] = stat

        if b + 1 < blocks:

            to_others(lambda where: send(stat_own.at[b], stat_all.at[b, di * tp + ti], b, STAT, where))
            unsent.append((tp * dp - 1, stat_own.at[b], b, STAT, None))
        else:
            to_tp(stat_own.at[b], stat_all.at[b, di * tp + ti], b, STAT)
            await_bytes(stat_all.at[b, pl.ds(0, tp - 1)], recv_sem.at[b, STAT])
            mean, scale = moments(stat_all[b, pl.ds(di * tp, tp)])
            result[...] = ((y - mean) * scale * gain_of(b, ti)).astype(bf16)

    for count, src, b, phase, also in unsent:
        each(count, lambda k: await_bytes(src, send_sem.at[b, phase]))
        if also is not None:

            @pl.when(also)
            def _():
                await_bytes(src, send_sem.at[b, phase])


def write_out(*refs):
    sem = refs[-1]
    copies = [pltpu.make_async_copy(refs[n], refs[4 + n], sem.at[n]) for n in (1, 2, 0, 3)]
    for copy in copies:
        copy.start()
    for copy in copies:
        copy.wait()


def shards(
    tp,
    dp,
    stream,
    query_weight,
    key_weight,
    value_weight,
    outgate_weight,
    gate_weight,
    gate_bias,
    output_weight,
    norm_gain,
    matrix_state,
    normalizer_state,
    stabilizer_state,
):
    blocks, seqs, chans, heads, size = matrix_state.shape
    feats = stream.shape[1]
    _, rows, cols = query_weight.shape
    ratio = tp // dp
    width = math.gcd(cols, size)
    pieces = cols // width
    if feats % 128:
        norm_gain = norm_gain.reshape(blocks, tp, feats)
    vmem = pltpu.VMEM
    far = pl.BlockSpec(memory_space=pltpu.HBM)
    held = pl.BlockSpec(memory_space=vmem)
    scratch = [
        vmem((seqs, feats), bf16),
        vmem((blocks, 4, rows, cols), bf16),
        vmem((blocks, 2 * heads, rows), bf16),
        vmem(gate_bias.shape, f32),
        vmem(output_weight.shape, bf16),
        vmem(norm_gain.shape, f32),
        vmem((blocks, ratio * dp, seqs, feats), bf16),
        vmem((blocks, dp, 2, seqs, cols), bf16),
        vmem((blocks, dp, 2, seqs, cols), bf16),
        vmem((blocks, dp, seqs, 2 * heads), f32),
        vmem((blocks, dp, seqs, 2 * heads), f32),
        vmem((blocks, dp, 2, seqs, cols), bf16),
        vmem((blocks, dp, 2, seqs, cols), bf16),
        vmem((blocks, 2, pieces, seqs, width), bf16),
        vmem((blocks, tp, 2, pieces, seqs, width), bf16),
        vmem((blocks, seqs, cols), bf16),
        vmem((blocks, ratio * dp, seqs, cols), bf16),
        vmem((blocks, dp, seqs, feats), bf16),
        vmem((blocks, dp, seqs, feats), bf16),
        vmem((blocks, 1, 128), f32),
        vmem((blocks, dp * tp, 1, 128), f32),
        vmem((blocks, seqs, feats), bf16),
        vmem((seqs, heads, size), f32),
        vmem((seqs, heads, size), f32),
        pltpu.SemaphoreType.DMA((5 + 7 * blocks,)),
        pltpu.SemaphoreType.DMA((blocks, 8)),
        pltpu.SemaphoreType.DMA((blocks, 8)),
    ]
    results = pl.pallas_call(
        functools.partial(kernel, tp, dp),
        out_shape=(
            vmem(stream.shape, bf16),
            vmem(matrix_state.shape, f32),
            vmem(normalizer_state.shape, f32),
            vmem(stabilizer_state.shape, f32),
        ),
        in_specs=[far] * 12,
        out_specs=(held,) * 4,
        scratch_shapes=scratch,
        compiler_params=pltpu.CompilerParams(
            collective_id=0, has_side_effects=True, vmem_limit_bytes=40 * 1024 * 1024
        ),
    )(*(
        pltpu.with_memory_space_constraint(operand, pltpu.HBM)
        for operand in (
        stream,
        query_weight,
        key_weight,
        value_weight,
        outgate_weight,
        jnp.swapaxes(gate_weight, 1, 2),
        gate_bias,
        output_weight,
        norm_gain,
        matrix_state,
        normalizer_state,
        stabilizer_state,
        )
    ))
    return pl.pallas_call(
        write_out,
        out_shape=tuple(jax.ShapeDtypeStruct(r.shape, r.dtype) for r in results),
        in_specs=[held] * 4,
        out_specs=(far,) * 4,
        scratch_shapes=[pltpu.SemaphoreType.DMA((4,))],
        compiler_params=pltpu.CompilerParams(vmem_limit_bytes=1024 * 1024),
    )(*results)


def solution(mesh):
    return jax.shard_map(
        functools.partial(shards, mesh.shape["tp"], mesh.shape["dp"]),
        mesh=mesh,
        in_specs=(
            P("dp", "tp"),
            P(None, "dp", "tp"),
            P(None, "dp", "tp"),
            P(None, "dp", "tp"),
            P(None, "dp", "tp"),
            P(),
            P(),
            P(None, "dp", "tp"),
            P(),
            P(None, "dp", "tp", None, None),
            P(None, "dp", None, None),
            P(None, "dp", None),
        ),
        out_specs=(
            P("dp", "tp"),
            P(None, "dp", "tp", None, None),
            P(None, "dp", None, None),
            P(None, "dp", None),
        ),
        check_vma=False,
    )
```
